32 devices in a mesh: sp: 8 (over z, core), tp: 4 (over y, x).
Axes of the slice: x: 2, y: 2, z: 4, core: 2. Of those that a mesh axis runs over, the one named last changes fastest.
Arguments:
- resid: bfloat16 [2048, 2048], P('sp'), may hold values from -18 to 18
- narrow_head_input: bfloat16 [2048, 1024], P('sp', 'tp'), may hold values from -6 to 6
- wide_head_input: bfloat16 [2048, 2048], P('sp', 'tp'), may hold values from -6 to 6
- key_group_input: bfloat16 [2048, 512], P('sp'), may hold values from -6 to 6
- query_group_input: bfloat16 [2048, 512], P('sp'), may hold values from -6 to 6
- narrow_output_gate: bfloat16 [2048, 1024], P('sp', 'tp'), may hold values from -6 to 6
- wide_output_gate: bfloat16 [2048, 2048], P('sp', 'tp'), may hold values from -6 to 6
- step_input_rows: bfloat16 [2048, 2, 16], P('sp', None, 'tp'), may hold values from -4 to 4
- head_decay_logarithm: float32 [2, 16], P(None, 'tp'), may hold values from -14 to -2
- position_log_decay: float32 [2048, 2, 16], P('sp', None, 'tp'), may hold values from -1.4 to 0
- direct_input_weight: float32 [2, 16], P(None, 'tp'), may hold values from 0.5 to 2
- narrow_conv_taps: float32 [4, 1024], P(None, 'tp'), may hold values from -3 to 3
- wide_conv_taps: float32 [4, 2048], P(None, 'tp'), may hold values from -3 to 3
- key_conv_taps: float32 [4, 512], replicated, may hold values from -3 to 3
- query_conv_taps: float32 [4, 512], replicated, may hold values from -3 to 3
- narrow_norm_gain: float32 [1024], P('tp'), may hold values from 0.1 to 1.9
- wide_norm_gain: float32 [2048], P('tp'), may hold values from 0.1 to 1.9
- narrow_output_rows: bfloat16 [1024, 2048], P('tp'), may hold values from -0.109375 to 0.109375
- wide_output_rows: bfloat16 [2048, 2048], P('tp'), may hold values from -0.109375 to 0.109375
- feedforward_norm_gain: float32 [2048], replicated, may hold values from 0.1 to 1.9
- routes: int32 [2048, 3], P('sp'), may hold values from 0 to 7, all different within a row; in each aligned block of 256 rows (0 to 255, 256 to 511, ...) at most 128 rows name the same one
- routing_weight_values: float32 [2048, 3], P('sp'), may hold values from 0.1 to 1
- expert_gate_matrix: bfloat16 [8, 2048, 2048], P('sp', None, 'tp'), may hold values from -1 to 1
- expert_up_matrix: bfloat16 [8, 2048, 2048], P('sp', None, 'tp'), may hold values from -1 to 1
- expert_down_matrix: bfloat16 [8, 2048, 2048], P('sp', 'tp'), may hold values from -0.015625 to 0.015625
Outputs:
- layer_out: bfloat16 [2048, 2048], P('sp', 'tp')
The draws below stay inside these ranges and needn't reach their ends.
Inputs may be any that keep to these rules, and one draw needn't show every extreme that they name: `routes`: each token names 3 different experts. Among the tokens of one index of sp (aligned blocks of 256 rows) no expert is named by more than 128 of them, and in some blocks one is named by exactly 128.
All inputs are finite; a program needn't handle non-finite values.
Results may differ from the reference program's by a relative error of at most 0.015.
Values may be sent and summed in bfloat16 or wider, within the bound.
No kernel may reach another device: no remote copies, remote signals or barrier semaphores. Data moves between devices by JAX's collectives and lax.ppermute only.
A program may use at most 64 MiB of HBM per device.

```python
import math
import jax
import jax.numpy as jnp
import numpy as np
from jax import lax

D = 2048
HEADS = 16
NARROW_HEAD_DIM = 64
WIDE_HEAD_DIM = 128
STATE = 128
GROUPS = 4
CONV_W = 4
BLOCK = 128
FF = 2048
TOPK = 3
TOK_SP = 256
TOKENS = 2048
EXPERTS = 8
CAP = 128
N_SP = 8
N_TP = 4


def draw_resid(key, part):
    key_base, key_rows = jax.random.split(jax.random.fold_in(key, 3), 2)
    row_scales = jnp.exp(jax.random.uniform(key_rows, (TOKENS, 1), jnp.float32, math.log(0.3), math.log(3.0)))
    base = jnp.clip(jax.random.normal(key_base, (TOKENS, D), jnp.float32), -6.0, 6.0)
    return jnp.clip(base * row_scales, -18.0, 18.0).astype(jnp.bfloat16)


def draw_step_input_rows(key, part):
    key_base, key_shift = jax.random.split(jax.random.fold_in(key, 5))
    block_total = TOKENS // TOK_SP
    shifts = jax.random.uniform(key_shift, (block_total, 1, 1, 1), jnp.float32, -1.0, 1.0)
    base = jax.random.normal(key_base, (block_total, TOK_SP, 2, HEADS), jnp.float32)
    return jnp.clip(base + shifts, -4.0, 4.0).reshape(TOKENS, 2, HEADS).astype(jnp.bfloat16)


def draw_head_decay_logarithm(key, part):
    key_kind, key_slow, key_fast = jax.random.split(jax.random.fold_in(key, 7), 3)
    slow_share = 0.5
    slow_heads = jax.random.uniform(key_kind, (2, HEADS), jnp.float32) < slow_share
    slow_rate = jnp.exp(jax.random.uniform(key_slow, (2, HEADS), jnp.float32, math.log(0.1), math.log(0.6))) / TOKENS
    fast_rate = jnp.exp(jax.random.uniform(key_fast, (2, HEADS), jnp.float32, math.log(1.0 / 60.0), math.log(1.0 / 20.0)))
    return jnp.clip(jnp.log(jnp.where(slow_heads, slow_rate, fast_rate)), -14.0, -2.0).astype(jnp.float32)


def draw_position_log_decay(key, part):
    key_spots, key_depth = jax.random.split(jax.random.fold_in(key, 9))
    spots = jax.random.randint(key_spots, (3,), 0, TOKENS)
    depth = jax.random.uniform(key_depth, (3, 2, HEADS), jnp.float32, math.log(0.5), math.log(0.8))
    hits = (jnp.arange(TOKENS)[:, None] == spots[None, :]).astype(jnp.float32)
    return jnp.clip(jnp.einsum('tk,khd->thd', hits, depth), -1.4, 0.0).astype(jnp.float32)


def draw_expert_gate_matrix(key, part):
    key_base, key_cols = jax.random.split(jax.random.fold_in(key, 11))
    column_scales = jnp.exp(jax.random.uniform(key_cols, (EXPERTS, 1, FF), jnp.float32, math.log(0.5), math.log(8.0)))
    base = jax.random.normal(key_base, (EXPERTS, D, FF), jnp.float32)
    return jnp.clip(base * column_scales / math.sqrt(D), -1.0, 1.0).astype(jnp.bfloat16)


def draw_expert_up_matrix(key, part):
    key_base, key_cols = jax.random.split(jax.random.fold_in(key, 13))
    column_scales = jnp.exp(jax.random.uniform(key_cols, (EXPERTS, 1, FF), jnp.float32, math.log(0.5), math.log(8.0)))
    base = jax.random.normal(key_base, (EXPERTS, D, FF), jnp.float32)
    return jnp.clip(base * column_scales / math.sqrt(D), -1.0, 1.0).astype(jnp.bfloat16)


def level_of(own_key, dims, shards, least, high):
    def one(dim, blocks):
        draws = jax.random.uniform(jax.random.fold_in(jax.random.fold_in(own_key, 6), dim), (blocks,), jnp.float32, least / len(shards), high / len(shards))
        return jnp.repeat(jnp.exp(draws), dims[dim] // blocks).reshape((-1,) + (1,) * (len(dims) - dim - 1))

    gain = one(*shards[0])
    for cut in shards[1:]:
        gain = gain * one(*cut)
    return gain


def shared_out(rng, own, number, rows, amount, top, limit, lean):
    sequence = jax.random.permutation(rng, amount)
    crowded, common = portions_of(amount, rows * top, limit, lean, True), portions_of(amount, rows * top, limit, lean, False)
    places = jnp.arange(amount)

    def named(tallies, offset_by):
        used = int((tallies > 0).sum())
        fixed = max(1, used // 4)
        moved = fixed + (places - fixed + offset_by * (used - fixed)) % max(1, amount - fixed)
        return jnp.zeros((amount,), jnp.int32).at[sequence[jnp.where(places < fixed, places, moved)]].set(jnp.asarray(tallies, jnp.int32))

    tallies = jnp.where(number % 4 == 0, named(crowded, number // 4), named(common, number - number // 4 - 1))
    mixed = jax.random.permutation(jax.random.fold_in(own, 3), amount)
    giver, sink = mixed[0:amount // 2 * 2:2], mixed[1:amount // 2 * 2:2]
    margin = jnp.minimum(tallies[giver] - 1, limit - tallies[sink]) // 2
    margin = jnp.where((giver == sequence[0]) | (sink == sequence[0]) | (tallies[sink] == 0), 0, jnp.maximum(margin, 0))
    moved = jax.random.randint(jax.random.fold_in(own, 4), (amount // 2,), 0, 1 << 20) % (margin + 1)
    tallies = tallies.at[giver].add(-moved).at[sink].add(moved)
    members = jnp.searchsorted(jnp.cumsum(tallies), jnp.arange(rows * top), side="right").astype(jnp.int32)
    listing = members.reshape(top, rows).T
    listing = listing[jax.random.permutation(jax.random.fold_in(own, 1), rows)]
    offset_by = jax.random.randint(jax.random.fold_in(own, 2), (rows, 1), 0, top)
    return jnp.take_along_axis(listing, (jnp.arange(top)[None, :] + offset_by) % top, axis=1)


def portions_of(number_of, total, bound, lean, full):
    portions = [(1 << 20) // math.isqrt(standing ** lean) + 1 for standing in range(1, number_of + 1)]
    largest = bound if full else min(bound, max(-(-total // number_of), total * portions[0] // sum(portions)))
    least = 1 if total - largest >= number_of - 1 else 0
    holding, surplus = [largest] + [least] * (number_of - 1), total - largest - least * (number_of - 1)
    while surplus > 0:
        movable = [i for i in range(1, number_of) if holding[i] < largest] or [i for i in range(1, number_of) if holding[i] < bound]
        pool, left = sum([portions[i] for i in movable]), surplus
        for i in movable:
            extra = min(bound - holding[i], max(1, left * portions[i] // pool), surplus)
            holding[i] = holding[i] + extra
            surplus = surplus - extra
    return np.array(holding)


def normal_values(rng, shape, deviation, limit, cuts=(), kind=jnp.bfloat16):
    drawn = deviation * jax.random.normal(rng, shape, jnp.float32)
    if cuts:
        drawn = drawn * level_of(rng, shape, cuts, -0.22, 0.18)
    return jnp.clip(drawn, -limit, limit).astype(kind)


def setup_inputs(seed: int = 0) -> dict:
    splits = jax.random.split(jax.random.key(seed), 26)
    resid = draw_resid(jax.random.fold_in(splits[25], 71), 0)
    narrow_head_input = normal_values(splits[1], (TOKENS, HEADS * NARROW_HEAD_DIM), 1.0, 6.0, ((0, 8), (1, 4)))
    wide_head_input = normal_values(splits[2], (TOKENS, HEADS * WIDE_HEAD_DIM), 1.0, 6.0, ((0, 8), (1, 4)))
    key_group_input = normal_values(splits[3], (TOKENS, GROUPS * STATE), 1.0, 6.0, ((0, 8),))
    query_group_input = normal_values(splits[4], (TOKENS, GROUPS * STATE), 1.0, 6.0, ((0, 8),))
    narrow_output_gate = normal_values(splits[5], (TOKENS, HEADS * NARROW_HEAD_DIM), 1.0, 6.0, ((0, 8), (1, 4)))
    wide_output_gate = normal_values(splits[6], (TOKENS, HEADS * WIDE_HEAD_DIM), 1.0, 6.0, ((0, 8), (1, 4)))
    step_input_rows = draw_step_input_rows(jax.random.fold_in(splits[25], 71), 0)
    head_decay_logarithm = draw_head_decay_logarithm(jax.random.fold_in(splits[25], 71), 0)
    position_log_decay = draw_position_log_decay(jax.random.fold_in(splits[25], 71), 0)
    direct_input_weight = jnp.clip(0.5 + 1.5 * jax.random.uniform(splits[10], (2, HEADS), jnp.float32) ** level_of(splits[10], (2, HEADS), ((1, 4),), -0.2, 0.2), 0.5, 2.0)
    narrow_conv_taps = normal_values(splits[11], (CONV_W, HEADS * NARROW_HEAD_DIM), CONV_W ** -0.5, 3.0, ((1, 4),), jnp.float32)
    wide_conv_taps = normal_values(splits[12], (CONV_W, HEADS * WIDE_HEAD_DIM), CONV_W ** -0.5, 3.0, ((1, 4),), jnp.float32)
    key_conv_taps = normal_values(splits[13], (CONV_W, GROUPS * STATE), CONV_W ** -0.5, 3.0, (), jnp.float32)
    query_conv_taps = normal_values(splits[14], (CONV_W, GROUPS * STATE), CONV_W ** -0.5, 3.0, (), jnp.float32)
    narrow_norm_gain = jnp.clip(1.0 + 0.18 * jax.random.normal(splits[15], (HEADS * NARROW_HEAD_DIM,), jnp.float32), 0.1, 1.9)
    wide_norm_gain = jnp.clip(1.0 + 0.18 * jax.random.normal(splits[16], (HEADS * WIDE_HEAD_DIM,), jnp.float32), 0.1, 1.9)
    narrow_output_rows = normal_values(splits[17], (HEADS * NARROW_HEAD_DIM, D), (HEADS * (NARROW_HEAD_DIM + WIDE_HEAD_DIM)) ** -0.5, 0.109375, ((0, 4),))
    wide_output_rows = normal_values(splits[18], (HEADS * WIDE_HEAD_DIM, D), (HEADS * (NARROW_HEAD_DIM + WIDE_HEAD_DIM)) ** -0.5, 0.109375, ((0, 4),))
    feedforward_norm_gain = jnp.clip(1.0 + 0.18 * jax.random.normal(splits[19], (D,), jnp.float32), 0.1, 1.9)
    routes_keys = jax.random.split(jax.random.fold_in(splits[20], 1), TOKENS // TOK_SP)
    routes_turns = jax.random.permutation(jax.random.fold_in(splits[20], 3), TOKENS // TOK_SP)
    routes = jax.vmap(lambda own, number: shared_out(jax.random.fold_in(splits[20], 2), own, number, TOK_SP, EXPERTS, TOPK, CAP, 1))(routes_keys, routes_turns).reshape((TOKENS, TOPK))
    routing_weight_values = jnp.clip(0.1 + 0.9 * jax.random.uniform(splits[21], (TOKENS, TOPK), jnp.float32) ** level_of(splits[21], (TOKENS, TOPK), ((0, 8),), -0.2, 0.2), 0.1, 1.0)
    expert_gate_matrix = draw_expert_gate_matrix(jax.random.fold_in(splits[25], 71), 0)
    expert_up_matrix = draw_expert_up_matrix(jax.random.fold_in(splits[25], 71), 0)
    expert_down_matrix = normal_values(splits[24], (EXPERTS, FF, D), (64 * FF) ** -0.5, 0.015625, ((0, 8), (1, 4)))
    return {"resid": resid, "narrow_head_input": narrow_head_input, "wide_head_input": wide_head_input, "key_group_input": key_group_input, "query_group_input": query_group_input, "narrow_output_gate": narrow_output_gate, "wide_output_gate": wide_output_gate, "step_input_rows": step_input_rows, "head_decay_logarithm": head_decay_logarithm, "position_log_decay": position_log_decay, "direct_input_weight": direct_input_weight, "narrow_conv_taps": narrow_conv_taps, "wide_conv_taps": wide_conv_taps, "key_conv_taps": key_conv_taps, "query_conv_taps": query_conv_taps, "narrow_norm_gain": narrow_norm_gain, "wide_norm_gain": wide_norm_gain, "narrow_output_rows": narrow_output_rows, "wide_output_rows": wide_output_rows, "feedforward_norm_gain": feedforward_norm_gain, "routes": routes, "routing_weight_values": routing_weight_values, "expert_gate_matrix": expert_gate_matrix, "expert_up_matrix": expert_up_matrix, "expert_down_matrix": expert_down_matrix}


NORM_EPS = 1e-06
CLAMP_LIMIT = 7.0
SIGMOID_SCALE = 1.702
FULL_PRECISION = lax.Precision.HIGHEST

def conv_with_rim(values, rim_rows, weight):
    length = values.shape[0]
    padded = jnp.concatenate([rim_rows, values], axis=0).astype(jnp.float32)
    accumulated = jnp.zeros((length, values.shape[1]), jnp.float32)
    for tap_index in range(weight.shape[0]):
        accumulated = accumulated + weight[tap_index] * padded[tap_index:tap_index + length]
    return jax.nn.silu(accumulated)

def pick_groups(channel_table, first_head, head_count):
    length = channel_table.shape[0]
    grouped = channel_table.reshape(length, GROUPS, -1)
    owners = (first_head + jnp.arange(head_count, dtype=jnp.int32)) // (HEADS // GROUPS)
    chooser = (owners[:, None] == jnp.arange(GROUPS, dtype=jnp.int32)[None, :]).astype(jnp.float32)
    return jnp.einsum('sgn,hg->shn', grouped, chooser, precision=FULL_PRECISION)

def local_head(values, step_logarithm, key_head_rows, query_head_rows, block_len):
    block_count = values.shape[0] // block_len
    values = values.reshape(block_count, block_len, -1)
    step_logarithm = step_logarithm.reshape(block_count, block_len)
    key_head_rows = key_head_rows.reshape(block_count, block_len, -1)
    query_head_rows = query_head_rows.reshape(block_count, block_len, -1)
    cum_decay = jnp.cumsum(step_logarithm, axis=1)
    causal_mask = jnp.arange(block_len)[:, None] >= jnp.arange(block_len)[None, :]
    decay_gaps = jnp.where(causal_mask[None], cum_decay[:, :, None] - cum_decay[:, None, :], -1e+30)
    scores = jnp.einsum('bln,bsn->bls', query_head_rows, key_head_rows, precision=FULL_PRECISION) * jnp.exp(decay_gaps)
    inside = jnp.einsum('bls,bsp->blp', scores, values, precision=FULL_PRECISION)
    tail_decay = jnp.exp(cum_decay[:, -1:] - cum_decay)
    states = jnp.einsum('bln,blp->bnp', key_head_rows * tail_decay[..., None], values, precision=FULL_PRECISION)
    totals = cum_decay[:, -1]

    def walk(running, member):
        return (jnp.exp(member[1]) * running + member[0], running)
    closing, entering = lax.scan(walk, jnp.zeros(states.shape[1:], jnp.float32), (states, totals))
    before = jnp.cumsum(totals) - totals
    return (inside, entering, closing, jnp.sum(totals), before, cum_decay, query_head_rows)

def finish_head(inside, entering, before, cum_decay, query_blocks, carried):
    starting = entering + jnp.exp(before)[:, None, None] * carried[None]
    readout = jnp.einsum('bln,bnp->blp', query_blocks * jnp.exp(cum_decay)[..., None], starting, precision=FULL_PRECISION)
    return (inside + readout).reshape(-1, inside.shape[-1])

def group_out(scanned, mixed_input_rows, direct_input_term, gate_input_rows, norm_gain_vector):
    length, head_count, head_dimension = mixed_input_rows.shape
    gated = jax.nn.silu(gate_input_rows.astype(jnp.float32)).reshape(length, head_count, head_dimension)
    result = (scanned + direct_input_term[None, :, None] * mixed_input_rows) * gated
    result = result * lax.rsqrt(lax.optimization_barrier(jnp.mean(result * result, axis=-1, keepdims=True)) + NORM_EPS)
    return (result.reshape(length, head_count * head_dimension) * norm_gain_vector).astype(jnp.bfloat16)

def mixer_head_group(unprojected_input, gate_input_rows, convolution_weight, key_head_table, query_head_table, unsoftened_step, decay_vector, position_decay_rows, direct_input_term, norm_gain_vector, head_dimension):
    length = unprojected_input.shape[0]
    zero_rim = jnp.zeros((convolution_weight.shape[0] - 1, unprojected_input.shape[1]), unprojected_input.dtype)
    mixed_input_rows = conv_with_rim(unprojected_input, zero_rim, convolution_weight).reshape(length, -1, head_dimension)
    head_count = mixed_input_rows.shape[1]
    key_head_rows = pick_groups(key_head_table, 0, head_count)
    query_head_rows = pick_groups(query_head_table, 0, head_count)
    step_length_values = jax.nn.softplus(unsoftened_step.astype(jnp.float32))
    step_logarithm = -jnp.exp(decay_vector)[None, :] * step_length_values + position_decay_rows
    values = mixed_input_rows * step_length_values[..., None]

    def one_head(head_values, head_log, head_keys, head_queries):
        parts = local_head(head_values, head_log, head_keys, head_queries, BLOCK)
        return finish_head(parts[0], parts[1], parts[4], parts[5], parts[6], jnp.zeros_like(parts[2]))
    scanned = jax.vmap(one_head, in_axes=(1, 1, 1, 1), out_axes=1)(values, step_logarithm, key_head_rows, query_head_rows)
    return group_out(scanned, mixed_input_rows, direct_input_term, gate_input_rows, norm_gain_vector)

def expert_layer(normed, routes, expert_gate_matrix, expert_up_matrix, expert_down_matrix):
    tokens = normed.shape[0]
    flat_routes = routes.reshape(-1).astype(jnp.int32)
    order_ids = jnp.argsort(flat_routes, stable=True).astype(jnp.int32)
    sorted_routes = flat_routes[order_ids]
    counts = lax.optimization_barrier(jnp.sum((flat_routes[:, None] == jnp.arange(EXPERTS, dtype=jnp.int32)[None, :]).astype(jnp.int32), axis=0))
    starts = (jnp.cumsum(counts) - counts).astype(jnp.int32)
    room = CAP * N_SP
    padded_ids = jnp.concatenate([order_ids, jnp.zeros((room,), jnp.int32)])

    def one_expert(member):
        start, gate_weight, up_weight, down_weight = member
        picked = lax.dynamic_slice_in_dim(padded_ids, start, room)
        rows = normed[picked // TOPK]
        gate_pre = jnp.dot(rows, gate_weight, preferred_element_type=jnp.float32)
        up_pre = jnp.dot(rows, up_weight, preferred_element_type=jnp.float32)
        clamped = jnp.minimum(gate_pre, CLAMP_LIMIT)
        act = ((jnp.clip(up_pre, -CLAMP_LIMIT, CLAMP_LIMIT) + 1.0) * clamped * jax.nn.sigmoid(SIGMOID_SCALE * clamped)).astype(jnp.bfloat16)
        pieces = act.reshape(room, N_TP, -1).astype(jnp.float32)
        blocks = down_weight.reshape(N_TP, -1, down_weight.shape[1]).astype(jnp.float32)
        partials = jnp.einsum('rtf,tfd->rtd', pieces, blocks)
        rounded = lax.optimization_barrier(partials.astype(jnp.bfloat16)).astype(jnp.float32)
        return lax.optimization_barrier(jnp.sum(rounded, axis=1)).astype(jnp.bfloat16)
    outputs = lax.map(one_expert, (starts, expert_gate_matrix, expert_up_matrix, expert_down_matrix))
    within = jnp.arange(tokens * TOPK, dtype=jnp.int32) - starts[sorted_routes]
    per_sorted = outputs.reshape(EXPERTS * room, -1)[sorted_routes * room + within]
    per_entry = jnp.zeros((tokens * TOPK, per_sorted.shape[1]), jnp.bfloat16).at[order_ids].set(per_sorted)
    return per_entry.reshape(tokens, TOPK, -1)

def reference(resid, narrow_head_input, wide_head_input, key_group_input, query_group_input, narrow_output_gate, wide_output_gate, step_input_rows, head_decay_logarithm, position_log_decay, direct_input_weight, narrow_conv_taps, wide_conv_taps, key_conv_taps, query_conv_taps, narrow_norm_gain, wide_norm_gain, narrow_output_rows, wide_output_rows, feedforward_norm_gain, routes, routing_weight_values, expert_gate_matrix, expert_up_matrix, expert_down_matrix):
    length = resid.shape[0]
    zero_rim = jnp.zeros((CONV_W - 1, key_group_input.shape[1]), key_group_input.dtype)
    key_head_table = conv_with_rim(key_group_input, zero_rim, key_conv_taps)
    query_head_table = conv_with_rim(query_group_input, zero_rim, query_conv_taps)
    narrow_head_output = mixer_head_group(narrow_head_input, narrow_output_gate, narrow_conv_taps, key_head_table, query_head_table, step_input_rows[:, 0], head_decay_logarithm[0], position_log_decay[:, 0], direct_input_weight[0], narrow_norm_gain, NARROW_HEAD_DIM)
    wide_head_output = mixer_head_group(wide_head_input, wide_output_gate, wide_conv_taps, key_head_table, query_head_table, step_input_rows[:, 1], head_decay_logarithm[1], position_log_decay[:, 1], direct_input_weight[1], wide_norm_gain, WIDE_HEAD_DIM)
    narrow_blocks = narrow_head_output.reshape(length, N_TP, -1).transpose(1, 0, 2)
    wide_blocks = wide_head_output.reshape(length, N_TP, -1).transpose(1, 0, 2)
    narrow_weights = narrow_output_rows.reshape(N_TP, -1, narrow_output_rows.shape[1])
    wide_weights = wide_output_rows.reshape(N_TP, -1, wide_output_rows.shape[1])

    def project(running, member):
        part_narrow, part_wide, weight_narrow, weight_wide = member
        term = jnp.dot(part_narrow, weight_narrow, preferred_element_type=jnp.float32)
        term = term + jnp.dot(part_wide, weight_wide, preferred_element_type=jnp.float32)
        return (running + lax.optimization_barrier(term.astype(jnp.bfloat16)).astype(jnp.float32), None)
    mixed, _ = lax.scan(project, jnp.zeros((length, narrow_output_rows.shape[1]), jnp.float32), (narrow_blocks, wide_blocks, narrow_weights, wide_weights))
    hidden_state = resid.astype(jnp.float32) + mixed
    normed = (hidden_state * lax.rsqrt(lax.optimization_barrier(jnp.mean(hidden_state * hidden_state, axis=-1, keepdims=True)) + NORM_EPS) * feedforward_norm_gain).astype(jnp.bfloat16)
    expert_rows = expert_layer(normed, routes, expert_gate_matrix, expert_up_matrix, expert_down_matrix)
    combined = lax.optimization_barrier(jnp.sum(expert_rows.astype(jnp.float32) * routing_weight_values[..., None], axis=1))
    return (hidden_state + combined).astype(jnp.bfloat16)
```

```python
import functools

import jax
import jax.numpy as jnp
from jax import lax
from jax.experimental import pallas as pl
from jax.experimental.pallas import tpu as pltpu
from jax.sharding import PartitionSpec as P

HEADS = 16
NARROW_HEAD_DIM = 64
WIDE_HEAD_DIM = 128
GROUPS = 4
STATE = 128
LANES = 128
CORES = 2

NORM_EPS = 1e-06
CLAMP_LIMIT = 7.0
SIGMOID_SCALE = 1.702
EXACT = lax.Precision.HIGHEST
F32 = jnp.float32
BF16 = jnp.bfloat16
VMEM = pl.BlockSpec(memory_space=pltpu.VMEM)
SMEM = pl.BlockSpec(memory_space=pltpu.SMEM)
ANY = pl.BlockSpec(memory_space=pl.ANY)


def dot(a, b, ca=1, cb=0, precision=None):
    return lax.dot_general(
        a, b, (((ca,), (cb,)), ((), ())), precision=precision, preferred_element_type=F32
    )


def iota(shape, dim):
    return lax.broadcasted_iota(jnp.int32, shape, dim)


def round_up(n, m):
    return (n + m - 1) // m * m


def silu(x):
    return x / (1.0 + jnp.exp(-x))


def call(body, outs, ins, scratch=(), flops=0, limit=56):
    single = not isinstance(outs, (list, tuple))
    outs = [outs] if single else list(outs)
    specs = [spec for spec, _ in ins]
    args = [a for _, a in ins]
    moved = sum(a.size * a.dtype.itemsize for a in args) + sum(
        o.size * o.dtype.itemsize for o in outs
    )
    res = pl.pallas_call(
        body,
        out_shape=outs,
        in_specs=specs,
        out_specs=[VMEM] * len(outs),
        scratch_shapes=list(scratch),
        compiler_params=pltpu.CompilerParams(vmem_limit_bytes=limit * 2**20),
        cost_estimate=pl.CostEstimate(
            flops=int(flops), bytes_accessed=int(moved), transcendentals=0
        ),
    )(*args)
    return res[0] if single else res


def sds(shape, dtype):
    return jax.ShapeDtypeStruct(shape, dtype)


class Heads:
    def __init__(self, count, length):
        self.count = count
        self.length = length
        self.narrow = count * NARROW_HEAD_DIM
        self.narrow_pad = round_up(self.narrow, LANES)
        self.wide = count * WIDE_HEAD_DIM
        self.width = self.narrow_pad + self.wide
        self.rows = round_up(2 * count, 8)
        per = LANES // NARROW_HEAD_DIM
        self.blocks = []
        for b in range(self.narrow_pad // LANES):
            members = []
            for h in range(b * per, min((b + 1) * per, count)):
                members.append((h, (h - b * per) * NARROW_HEAD_DIM))
            self.blocks.append((b * LANES, members))
        for h in range(count):
            self.blocks.append((self.narrow_pad + h * WIDE_HEAD_DIM, [(count + h, None)]))

    def spread(self):
        col = iota((self.rows, self.width), 1)
        row = iota((self.rows, self.width), 0)
        narrow = jnp.where(col < self.narrow, col // NARROW_HEAD_DIM, -1)
        wide = self.count + (col - self.narrow_pad) // WIDE_HEAD_DIM
        return (jnp.where(col < self.narrow_pad, narrow, wide) == row).astype(F32)

    def member(self, block, lane):
        if lane is None:
            return block
        at = iota(block.shape, 1)
        return jnp.where((at >= lane) & (at < lane + NARROW_HEAD_DIM), block, 0.0)


def upper(n):
    return (iota((n, n), 0) <= iota((n, n), 1)).astype(F32)


def mix_body(hd, rim_at, c_ref, nar, wid, key, qry, rim, tn, tw, tk, tq, a_t, step_t,
             x_out, b_out, c_out, keep, send, pad, states):
    length = hd.length
    x_out[...] = jnp.zeros(x_out.shape, F32)

    def conv(src, taps, at):
        width = src.shape[1]
        pad[0:8, :width] = rim[:, at : at + width].astype(F32)
        pad[8 : 8 + length, :width] = src[...].astype(F32)
        count = taps.shape[0]
        acc = jnp.zeros((length, width), F32)
        for j in range(count):
            acc = acc + taps[j : j + 1, :] * pad[9 - count + j : 9 - count + j + length, :width]
        return silu(acc)

    x_out[:, : hd.narrow] = conv(nar, tn, rim_at[0])
    x_out[:, hd.narrow_pad :] = conv(wid, tw, rim_at[1])
    keys = conv(key, tk, rim_at[2])
    b_out[...] = keys.astype(BF16)
    c_out[...] = conv(qry, tq, rim_at[3]).astype(BF16)
    cum = dot(a_t[...], upper(length), precision=EXACT)
    total = cum[:, length - 1 : length]
    weight = jnp.exp(total - cum) * step_t[...]
    keys_t = keys.T
    for at, members in hd.blocks:
        block = x_out[:, at : at + LANES]
        acc = jnp.zeros((STATE, LANES), F32)
        for h, lane in members:
            acc = acc + dot(
                (keys_t * weight[h : h + 1, :]).astype(BF16), hd.member(block, lane).astype(BF16)
            )
        states[:, at : at + LANES] = acc
    spread = jnp.sum(hd.spread() * total, axis=0, keepdims=True)
    high = spread.astype(BF16).astype(F32)
    row = iota((16, hd.width), 0)
    tail = jnp.where(row == 0, high, jnp.where(row == 1, spread - high, 0.0)).astype(BF16)
    half = STATE // CORES
    core = c_ref[0]
    mine = pl.multiple_of(core * half, half)
    other = pl.multiple_of((1 - core) * half, half)
    keep[0:half, :] = states[pl.ds(mine, half), :].astype(BF16)
    send[0:half, :] = states[pl.ds(other, half), :].astype(BF16)
    keep[half:, :] = tail
    send[half:, :] = tail


def inner_body(hd, x, b, c, a_t, step_t, direct, y_out):
    length = hd.length
    cum = dot(a_t[...], upper(length), precision=EXACT)
    lower = (iota((length, length), 0) >= iota((length, length), 1)).astype(F32)
    cum_col = dot(lower, a_t[...], 1, 1, precision=EXACT)
    causal = iota((length, length), 0) >= iota((length, length), 1)
    scores = dot(c[...], b[...], 1, 1)
    skip = jnp.sum(hd.spread() * direct[...], axis=0, keepdims=True)
    for at, members in hd.blocks:
        block = x[:, at : at + LANES]
        acc = skip[:, at : at + LANES] * block
        for h, lane in members:
            gap = jnp.where(causal, cum_col[:, h : h + 1] - cum[h : h + 1, :], -1e30)
            m = scores * jnp.exp(gap) * step_t[h : h + 1, :]
            acc = acc + dot(m.astype(BF16), hd.member(block, lane).astype(BF16))
        y_out[:, at : at + LANES] = acc


def project_body(hd, tp, s_ref, y, c, own, got, a_t, gate_n, gate_w, gain_n, gain_w, rows_n, rows_w, *rest):
    outs, (carry, normed) = rest[:tp], rest[tp:]
    length = hd.length
    half = STATE // CORES
    core = s_ref[0]
    place = s_ref[1]
    carry[pl.ds(pl.multiple_of(core * half, half), half), :] = own[...].astype(F32)
    carry[pl.ds(pl.multiple_of((1 - core) * half, half), half), :] = got[...].astype(F32)
    lower = (iota((length, length), 0) >= iota((length, length), 1)).astype(F32)
    cum_col = dot(lower, a_t[...], 1, 1, precision=EXACT)
    spread = hd.spread()
    decay = dot(jnp.exp(cum_col), spread, precision=EXACT)
    total = y[...] + decay * dot(c[...], carry[...].astype(BF16))

    def finish(part, gate, gain, dim):
        part = part * silu(gate[...].astype(F32))
        width = part.shape[1]
        col = iota((width, LANES), 0) // dim
        pick = (col == iota((width, LANES), 1)).astype(F32)
        mean = dot(part * part, pick, precision=EXACT) * (1.0 / dim)
        scale = dot(lax.rsqrt(mean + NORM_EPS), pick, 1, 1, precision=EXACT)
        return (part * scale * gain[...]).astype(BF16)

    out_n = finish(total[:, : hd.narrow], gate_n, gain_n, NARROW_HEAD_DIM)
    out_w = finish(total[:, hd.narrow_pad :], gate_w, gain_w, WIDE_HEAD_DIM)
    width = outs[0].shape[1]
    for d in range(tp):
        at = pl.multiple_of((place ^ d) * width, LANES)
        part = dot(out_n, rows_n[:, pl.ds(at, width)]) + dot(out_w, rows_w[:, pl.ds(at, width)])
        outs[d][...] = part.astype(BF16)


def hidden_body(tp, s_ref, resid, gain, *rest):
    parts, (hidden_out, pay_out) = rest[:tp], rest[tp:]
    length, width = parts[0].shape
    at = pl.multiple_of(s_ref[1] * width, LANES)
    hidden = resid[:, pl.ds(at, width)].astype(F32)
    total = parts[0][...].astype(F32)
    for part in parts[1:]:
        total = total + part[...].astype(F32)
    hidden = hidden + total
    hidden_out[...] = hidden
    pay_out[0:length, :] = (hidden * gain[:, pl.ds(at, width)]).astype(BF16)
    squares = dot(jnp.ones((8, width), F32), hidden * hidden, 1, 1, precision=EXACT)
    pay_out[length:, :] = jnp.zeros((pay_out.shape[0] - length, width), BF16)
    step = min(length, width)
    for i in range(length // step):
        piece = squares[0:1, i * step : (i + 1) * step]
        high = piece.astype(BF16)
        pay_out[length + i : length + i + 1, 0:step] = high
        pay_out[length + 8 + i : length + 9 + i, 0:step] = (piece - high.astype(F32)).astype(BF16)


def hits_of(rt, expert, picks):
    hit = jnp.zeros((1, rt.shape[1]), F32)
    load = jnp.zeros((1, rt.shape[1]), F32)
    for k in range(picks):
        match = (rt[k : k + 1, :] == expert).astype(F32)
        hit = hit + match
        load = load + match * rt[picks + k : picks + k + 1, :]
    return hit, load


def slots_of(hit, cap):
    length = hit.shape[1]
    before = (iota((length, length), 0) < iota((length, length), 1)).astype(BF16)
    rank = dot(jnp.broadcast_to(hit, (8, length)).astype(BF16), before)[0:1, :]
    slot = iota((cap, length), 0).astype(F32)
    return jnp.where((rank == slot) & (hit > 0.5), 1.0, 0.0)


def select_body(n, cap, picks, s_ref, *rest):
    pays, rts, outs = rest[:n], rest[n : 2 * n], rest[2 * n :]
    length = rts[0].shape[1]
    width = pays[0].shape[1]
    step = min(length, width)
    for out in outs:
        out[n * cap :, :] = jnp.zeros((out.shape[0] - n * cap, width), BF16)
    for i in range(n):
        rt = rts[i][...]
        block = pays[i][0:length, :]
        pieces = []
        for j in range(length // step):
            high = pays[i][length + j : length + j + 1, 0:step].astype(F32)
            low = pays[i][length + 8 + j : length + 9 + j, 0:step].astype(F32)
            pieces.append(high + low)
        squares = pieces[0] if len(pieces) == 1 else jnp.concatenate(pieces, axis=1)
        squares = jnp.broadcast_to(squares, (8, length))
        for which, out in enumerate(outs):
            hit, _ = hits_of(rt, s_ref[2 + which].astype(F32), picks)
            onehot = slots_of(hit, cap)
            out[i * cap : (i + 1) * cap, :] = dot(onehot.astype(BF16), block).astype(BF16)
            ssq = dot(squares, onehot, 1, 1, precision=EXACT)[0:1, :]
            high = ssq.astype(BF16)
            out[n * cap + i : n * cap + i + 1, 0:cap] = high
            out[n * cap + n + i : n * cap + n + i + 1, 0:cap] = (ssq - high.astype(F32)).astype(BF16)


def expert_body(tp, n, cap, model, s_ref, *rest):
    xs, weights, outs = rest[:tp], rest[tp : tp + 9], rest[tp + 9 : 2 * tp + 9]
    bufs, sems = rest[2 * tp + 9 : 2 * tp + 15], rest[2 * tp + 15]
    own, first, second = weights[0:3], weights[3:6], weights[6:9]
    native = s_ref[4]

    def start(source, q):
        for m in range(3):
            pltpu.make_async_copy(source[m], bufs[3 * q + m], sems.at[3 * q + m]).start()

    @pl.when(native == 1)
    def _():
        start(own, 0)
        start(first, 1)

    @pl.when(native == 0)
    def _():
        start(first, 0)
        start(second, 1)

    def arrive(q, m):
        pltpu.make_async_copy(own[m], bufs[3 * q + m], sems.at[3 * q + m]).wait()

    place = s_ref[1]
    width = xs[0].shape[1]
    eye = (iota((cap, cap), 0) == iota((cap, cap), 1)).astype(F32)
    scales = []
    for i in range(n):
        ssq = jnp.zeros((1, cap), F32)
        for x in xs:
            ssq = ssq + x[n * cap + i : n * cap + i + 1, 0:cap].astype(F32)
            ssq = ssq + x[n * cap + n + i : n * cap + n + i + 1, 0:cap].astype(F32)
        col = dot(eye, jnp.broadcast_to(ssq, (8, cap)), 1, 1, precision=EXACT)[:, 0:1]
        scales.append(lax.rsqrt(col * (1.0 / model) + NORM_EPS))
    scale = jnp.concatenate(scales, axis=0) if n > 1 else scales[0]

    def product(buf):
        acc = None
        for d in range(tp):
            at = pl.multiple_of((place ^ d) * width, LANES)
            part = dot(xs[d][0 : n * cap, :], buf[pl.ds(at, width), :])
            acc = part if acc is None else acc + part
        return acc * scale

    acts = []
    for q in range(CORES):
        arrive(q, 0)
        gate = jnp.minimum(product(bufs[3 * q]), CLAMP_LIMIT)
        arrive(q, 1)
        up = jnp.clip(product(bufs[3 * q + 1]), -CLAMP_LIMIT, CLAMP_LIMIT)
        act = (up + 1.0) * gate / (1.0 + jnp.exp(-SIGMOID_SCALE * gate))
        acts.append(act.astype(BF16))
    for q in range(CORES):
        arrive(q, 2)
    for d in range(tp):
        at = pl.multiple_of((place ^ d) * width, LANES)
        part = None
        for q in range(CORES):
            one = dot(acts[q], bufs[3 * q + 2][:, pl.ds(at, width)])
            part = one if part is None else part + one
        outs[d][...] = part.astype(BF16)


def combine_body(tp, n, cap, picks, s_ref, *rest):
    parts, rts, outs = rest[:tp], rest[tp : tp + n], rest[tp + n :]
    for i in range(n):
        rt = rts[i][...]
        rows = slice(i * cap, (i + 1) * cap)
        total = None
        for which in range(2):
            group = parts[: tp // 2] if which == 0 else parts[tp // 2 :]
            value = group[0][rows, :].astype(F32)
            for part in group[1:]:
                value = value + part[rows, :].astype(F32)
            hit, load = hits_of(rt, s_ref[2 + which].astype(F32), picks)
            placed = slots_of(hit, cap) * load
            one = dot(placed, value, 0, 0, precision=EXACT)
            total = one if total is None else total + one
        outs[i][...] = total.astype(BF16)


def local(
    resid,
    narrow_head_input,
    wide_head_input,
    key_group_input,
    query_group_input,
    narrow_output_gate,
    wide_output_gate,
    step_input_rows,
    head_decay_logarithm,
    position_log_decay,
    direct_input_weight,
    narrow_conv_taps,
    wide_conv_taps,
    key_conv_taps,
    query_conv_taps,
    narrow_norm_gain,
    wide_norm_gain,
    narrow_output_rows,
    wide_output_rows,
    feedforward_norm_gain,
    routes,
    routing_weight_values,
    expert_gate_matrix,
    expert_up_matrix,
    expert_down_matrix,
):
    sp, tp = lax.axis_size("sp"), lax.axis_size("tp")
    chips = sp // CORES
    sp_at, tp_at = lax.axis_index("sp"), lax.axis_index("tp")
    chip, core = sp_at // CORES, sp_at % CORES
    side = tp_at // (tp // 2)
    native = (side == core).astype(jnp.int32)
    length, model = resid.shape
    width = model // tp
    hd = Heads(narrow_head_input.shape[1] // NARROW_HEAD_DIM, length)
    picks = routes.shape[1]
    cap = 4 * length * picks // (3 * sp)
    scalars = jnp.stack(
        [core, tp_at, CORES * chip + side, CORES * chip + 1 - side, native]
    ).astype(jnp.int32)

    def shift(x, by):
        return lax.ppermute(x, "sp", [(i, i + by) for i in range(sp - by)])

    def flip(x, axis, size, bits):
        return lax.ppermute(x, axis, [(i, i ^ bits) for i in range(size)])

    def over_z(x, d):
        return flip(x, "sp", sp, CORES * d)

    def over_tp(x, d):
        return flip(x, "tp", tp, d)

    def to_partner(x):
        return flip(x, "sp", sp, 1)

    group = tp_at * hd.count // (HEADS // GROUPS)
    key_in = lax.dynamic_slice_in_dim(key_group_input, group * STATE, STATE, 1)
    query_in = lax.dynamic_slice_in_dim(query_group_input, group * STATE, STATE, 1)
    key_taps = lax.dynamic_slice_in_dim(key_conv_taps, group * STATE, STATE, 1)
    query_taps = lax.dynamic_slice_in_dim(query_conv_taps, group * STATE, STATE, 1)
    pieces, rim_at, at = [], [], 0
    for src in (narrow_head_input, wide_head_input, key_in, query_in):
        last = src[length - 8 :]
        extra = round_up(last.shape[1], LANES) - last.shape[1]
        pieces.append(jnp.pad(last, ((0, 0), (0, extra))) if extra else last)
        rim_at.append(at)
        at += last.shape[1] + extra
    rim = shift(jnp.concatenate(pieces, axis=1), 1)

    mats = (expert_gate_matrix[0], expert_up_matrix[0], expert_down_matrix[0])
    swap, share = [], []
    for s in range(sp):
        for t in range(tp):
            if t // (tp // 2) == s % CORES:
                swap.append((s * tp + t, (s ^ 1) * tp + t))
                share.append((s * tp + t, (s ^ 1) * tp + t))
            else:
                swap.append((s * tp + t, s * tp + (t ^ (tp // 2))))
    first = [lax.ppermute(m, ("sp", "tp"), swap) for m in mats]
    second = [lax.ppermute(m, ("sp", "tp"), share) for m in first]

    table = jnp.concatenate([routes.T.astype(F32), routing_weight_values.T], axis=0)
    table = jnp.pad(table, ((0, round_up(2 * picks, 8) - 2 * picks), (0, 0)))
    tables = [table] + [over_z(table, d) for d in range(1, chips)]

    def by_head(a):
        rows = jnp.transpose(a, (1, 2, 0)).reshape(2 * hd.count, -1)
        return jnp.pad(rows, ((0, hd.rows - 2 * hd.count), (0, 0)))

    step_t = jax.nn.softplus(step_input_rows.astype(F32))
    decay_t = -jnp.exp(head_decay_logarithm)[None] * step_t + position_log_decay
    step_t, decay_t = by_head(step_t), by_head(decay_t)
    direct = by_head(direct_input_weight[None])

    wide_cols = max(hd.narrow, hd.wide, STATE)
    half = STATE // CORES
    x, b, c, keep, send = call(
        functools.partial(mix_body, hd, tuple(rim_at)),
        [
            sds((length, hd.width), F32),
            sds((length, STATE), BF16),
            sds((length, STATE), BF16),
            sds((half + 16, hd.width), BF16),
            sds((half + 16, hd.width), BF16),
        ],
        [
            (SMEM, scalars),
            (VMEM, narrow_head_input),
            (VMEM, wide_head_input),
            (VMEM, key_in),
            (VMEM, query_in),
            (VMEM, rim),
            (VMEM, narrow_conv_taps),
            (VMEM, wide_conv_taps),
            (VMEM, key_taps),
            (VMEM, query_taps),
            (VMEM, decay_t),
            (VMEM, step_t),
        ],
        [pltpu.VMEM((length + 8, wide_cols), F32), pltpu.VMEM((STATE, hd.width), F32)],
        flops=2e9,
    )

    got = to_partner(send)
    early = jnp.where(core == 0, keep, got).astype(F32)
    late = jnp.where(core == 0, got, keep).astype(F32)

    def parts_of(p):
        return p[:half], p[half : half + 1] + p[half + 1 : half + 2]

    state_0, total_0 = parts_of(early)
    state_1, total_1 = parts_of(late)
    both = total_0 + total_1
    high = both.astype(BF16)
    low = (both - high.astype(F32)).astype(BF16)
    chip_pay = jnp.concatenate(
        [
            (jnp.exp(total_1) * state_0 + state_1).astype(BF16),
            high,
            low,
            jnp.zeros((14, hd.width), BF16),
        ],
        axis=0,
    )
    arrived = [shift(chip_pay, CORES * d) for d in range(1, chips)]

    y = call(
        functools.partial(inner_body, hd),
        sds((length, hd.width), F32),
        [(VMEM, x), (VMEM, b), (VMEM, c), (VMEM, decay_t), (VMEM, step_t), (VMEM, direct)],
        flops=4e9,
    )

    carry = jnp.zeros((half, hd.width), F32)
    passed = jnp.zeros((1, hd.width), F32)
    for one in arrived:
        state, total = parts_of(one.astype(F32))
        carry = carry + jnp.exp(passed) * state
        passed = passed + total
    carry_0 = carry
    carry_1 = jnp.exp(total_0) * carry + state_0
    own_carry = jnp.where(core == 0, carry_0, carry_1).astype(BF16)
    other_carry = to_partner(jnp.where(core == 0, carry_1, carry_0).astype(BF16))

    parts = call(
        functools.partial(project_body, hd, tp),
        [sds((length, width), BF16)] * tp,
        [
            (SMEM, scalars),
            (VMEM, y),
            (VMEM, c),
            (VMEM, own_carry),
            (VMEM, other_carry),
            (VMEM, decay_t),
            (VMEM, narrow_output_gate),
            (VMEM, wide_output_gate),
            (VMEM, narrow_norm_gain[None]),
            (VMEM, wide_norm_gain[None]),
            (VMEM, narrow_output_rows),
            (VMEM, wide_output_rows),
        ],
        [pltpu.VMEM((STATE, hd.width), F32), pltpu.VMEM((8, LANES), F32)],
        flops=2e9,
    )
    parts = [parts[0]] + [over_tp(parts[d], d) for d in range(1, tp)]

    hidden, pay = call(
        functools.partial(hidden_body, tp),
        [sds((length, width), F32), sds((length + 16, width), BF16)],
        [(SMEM, scalars), (VMEM, resid), (VMEM, feedforward_norm_gain[None])]
        + [(VMEM, p) for p in parts],
        flops=1e9,
    )
    pays = [pay] + [over_z(pay, d) for d in range(1, chips)]

    groups = 2
    per = chips // groups
    out = hidden
    for g in range(groups):
        members = range(g * per, (g + 1) * per)
        n = len(members)
        rows = n * cap + round_up(2 * n, 16)
        same, other = call(
            functools.partial(select_body, n, cap, picks),
            [sds((rows, width), BF16)] * 2,
            [(SMEM, scalars)]
            + [(VMEM, pays[d]) for d in members]
            + [(VMEM, tables[d]) for d in members],
            flops=1e9,
        )
        xs = [same] + [over_tp(same if d < tp // 2 else other, d) for d in range(1, tp)]
        ff = mats[0].shape[1]
        results = call(
            functools.partial(expert_body, tp, n, cap, model),
            [sds((n * cap, width), BF16)] * tp,
            [(SMEM, scalars)]
            + [(VMEM, a) for a in xs]
            + [(ANY, a) for a in (*mats, *first, *second)],
            [pltpu.VMEM(m.shape, BF16) for m in (*mats, *mats)] + [pltpu.SemaphoreType.DMA((6,))],
            flops=12 * n * cap * model * ff,
        )
        results = [results[0]] + [over_tp(results[d], d) for d in range(1, tp)]
        sums = call(
            functools.partial(combine_body, tp, n, cap, picks),
            [sds((length, width), BF16)] * n,
            [(SMEM, scalars)]
            + [(VMEM, a) for a in results]
            + [(VMEM, tables[d]) for d in members],
            flops=1e9,
        )
        for d, one in zip(members, sums):
            out = out + (over_z(one, d) if d else one).astype(F32)
    return out.astype(BF16)


def solution(mesh):
    return jax.shard_map(
        local,
        mesh=mesh,
        in_specs=(
            P("sp", None),
            P("sp", "tp"),
            P("sp", "tp"),
            P("sp", None),
            P("sp", None),
            P("sp", "tp"),
            P("sp", "tp"),
            P("sp", None, "tp"),
            P(None, "tp"),
            P("sp", None, "tp"),
            P(None, "tp"),
            P(None, "tp"),
            P(None, "tp"),
            P(),
            P(),
            P("tp"),
            P("tp"),
            P("tp", None),
            P("tp", None),
            P(),
            P("sp", None),
            P("sp", None),
            P("sp", None, "tp"),
            P("sp", None, "tp"),
            P("sp", "tp", None),
        ),
        out_specs=P("sp", "tp"),
        check_vma=False,
    )
```
